32 devices in a mesh: fs: 8 (over z, y), tp: 4 (over x, core).
Axes of the slice: x: 2, y: 2, z: 4, core: 2. Of those that a mesh axis runs over, the one named last changes fastest.
Arguments:
- inputs: bfloat16 [48, 4096], P('fs', 'tp'), may hold values from -0.875 to 0.875
- cotangent: bfloat16 [48, 4096], P('fs', 'tp'), may hold values from -8 to 8
- pre_act: bfloat16 [48, 16384], P(None, 'fs'), may hold values from -3 to 3
- w_up: bfloat16 [4096, 16384], P('tp', 'fs'), may hold values from -0.046875 to 0.046875
- w_down: bfloat16 [16384, 4096], P('fs', 'tp'), may hold values from -0.09375 to 0.09375
Outputs:
- grad_input: bfloat16 [48, 4096], P('fs', 'tp')
- grad_up: float32 [4096, 16384], P('tp', 'fs')
- grad_down: float32 [16384, 4096], P('fs', 'tp')
The draws below stay inside these ranges and needn't reach their ends.
All inputs are finite; a program needn't handle non-finite values.
Results may differ from the reference program's by a relative error of at most 0.017.
Values may be sent and summed in bfloat16 or wider, within the bound.
A program may use at most 64 MiB of HBM per device.

```python
import jax
import jax.numpy as jnp

D = 4096
FF = 16384
TOKENS = 48


def spiked(drawn, rng, source, target, blocks, factor):
    def block_of(dim):
        return (jnp.arange(drawn.shape[dim]) // (drawn.shape[dim] // blocks)).reshape((-1,) + (1,) * (drawn.ndim - 1 - dim))

    near = jax.random.permutation(rng, blocks)[block_of(target)]
    second = (block_of(target) + blocks // 2) % blocks
    return jnp.where((block_of(source) == near) | (block_of(source) == second), factor * drawn, drawn)


def shard_levels(rng, extent, pieces, smallest, largest):
    gain, own = 1.0, jax.random.fold_in(rng, 6)
    for axis_at, parts in pieces:
        heights = jnp.exp(jax.random.uniform(jax.random.fold_in(own, axis_at), (parts,), jnp.float32, smallest / len(pieces), largest / len(pieces)))
        gain = gain * jnp.repeat(heights, extent[axis_at] // parts).reshape([-1 if axis == axis_at else 1 for axis in range(len(extent))])
    return gain


def bell_draw(stream_key, shape, deviation, most, shards=(), kind=jnp.bfloat16):
    drawn = deviation * jax.random.normal(stream_key, shape, jnp.float32)
    if shards:
        drawn = drawn * shard_levels(stream_key, shape, shards, -0.22, 0.18)
    return jnp.clip(drawn, -most, most).astype(kind)


def gaussian_with(rng, dims, deviation, bound, cuts, heavy, kind=jnp.bfloat16):
    entries = deviation * jax.random.normal(rng, dims, jnp.float32)
    if cuts:
        entries = entries * shard_levels(rng, dims, cuts, -0.22, 0.18)
    return jnp.clip(spiked(entries, jax.random.fold_in(rng, 3), *heavy), -bound, bound).astype(kind)


def setup_inputs(seed: int = 0) -> dict:
    key_list = jax.random.split(jax.random.key(seed), 6)
    inputs = bell_draw(key_list[0], (TOKENS, D), (TOKENS ** -0.5), 0.875, ((0, 8), (1, 4)))
    cotangent = gaussian_with(key_list[1], (TOKENS, D), 1.0, 8.0, ((0, 8), (1, 4)), (0, 1, 8, 2.0))
    pre_act = gaussian_with(key_list[2], (TOKENS, FF), (TOKENS ** -0.25), 3.0, ((1, 8),), (1, 0, 8, 2.0))
    w_up = bell_draw(key_list[3], (D, FF), FF ** -0.5, 0.046875, ((0, 4), (1, 8)))
    w_down = bell_draw(key_list[4], (FF, D), D ** -0.5, 0.09375, ((0, 8), (1, 4)))
    return {"inputs": inputs, "cotangent": cotangent, "pre_act": pre_act, "w_up": w_up, "w_down": w_down}


def reference(inputs, cotangent, pre_act, w_up, w_down):
    active = jax.nn.relu(pre_act.astype(jnp.float32))
    act = jnp.square(active).astype(jnp.bfloat16)
    hidden = jnp.dot(cotangent, w_down.T, preferred_element_type=jnp.float32)
    grad_pre = (2.0 * active * hidden).astype(jnp.bfloat16)
    grad_down = jnp.dot(act.T, cotangent, preferred_element_type=jnp.float32)
    grad_up = jnp.dot(inputs.T, grad_pre, preferred_element_type=jnp.float32)
    grad_input = jnp.dot(grad_pre, w_up.T, preferred_element_type=jnp.float32).astype(jnp.bfloat16)
    return grad_input, grad_up, grad_down
```

```python
import functools

import jax
import jax.numpy as jnp
from jax import lax
from jax.experimental import pallas as pl
from jax.experimental.pallas import tpu as pltpu
from jax.sharding import PartitionSpec as P

F32, BF16 = jnp.float32, jnp.bfloat16
SLAB = 8
NT = (((1,), (1,)), ((), ()))
TN = (((0,), (0,)), ((), ()))
NN = (((1,), (0,)), ((), ()))


def dot(a, b, dims):
    return lax.dot_general(a, b, dims, preferred_element_type=F32)


def exchange(
    n,
    chips,
    chunks,
    cot_ref,
    in_ref,
    pre_ref,
    wu_ref,
    wd_ref,
    cot_out,
    in_out,
    gp_out,
    gi_out,
    cot_v,
    in_v,
    pre_v,
    wu_v,
    wd_v,
    cot_g,
    in_g,
    spread,
    own,
    p1_s,
    p1_r,
    p2_s,
    p2_r,
    rs_s,
    rs_r,
    local,
    cs,
    cr,
    is_,
    ir,
    s1,
    r1,
    s2,
    r2,
    s3,
    r3,
    s4,
    r4,
):
    me = lax.axis_index("fs")
    tp = lax.axis_index("tp")
    core = lax.rem(tp, 2)
    rows = cot_v.shape[0]
    tokens = n * rows
    width = wd_v.shape[1]
    fs_peer = [None] + [lax.rem(me + k, n) for k in range(1, n)]
    partner = tp + 1 - 2 * core
    x_peer = [None] + [lax.rem(tp + 2 * k, 2 * chips) for k in range(1, chips)]
    targets = (
        [{"fs": p} for p in fs_peer[1:]]
        + [{"tp": partner}]
        + [{"tp": p} for p in x_peer[1:]]
    )

    barrier = pltpu.get_barrier_semaphore()
    for t in targets:
        pl.semaphore_signal(barrier, inc=1, device_id=t)

    load_cot = pltpu.make_async_copy(cot_ref, cot_v, local.at[0])
    load_in = pltpu.make_async_copy(in_ref, in_v, local.at[1])
    load_cot.start()
    load_in.start()
    load_wd, load_pre, load_wu = [], [], []
    for j in range(2 * chunks):
        load_wd.append(
            pltpu.make_async_copy(
                wd_ref.at[pl.ds(j * width, width)], wd_v.at[j], local.at[4 + j]
            )
        )
        load_wd[-1].start()
    for j in range(2 * chunks):
        load_pre.append(
            pltpu.make_async_copy(
                pre_ref.at[:, pl.ds(j * width, width)],
                pre_v.at[j],
                local.at[4 + 2 * chunks + j],
            )
        )
        load_pre[-1].start()
    for j in range(2 * chunks):
        load_wu.append(
            pltpu.make_async_copy(
                wu_ref.at[:, pl.ds(j * width, width)],
                wu_v.at[j],
                local.at[4 + 4 * chunks + j],
            )
        )
        load_wu[-1].start()
    spread[...] = jnp.zeros_like(spread)
    load_cot.wait()
    load_in.wait()
    own_cot = pltpu.make_async_copy(cot_v, cot_g.at[me], local.at[2])
    own_in = pltpu.make_async_copy(in_v, in_g.at[me], local.at[3])
    own_cot.start()
    own_in.start()

    pl.semaphore_wait(barrier, len(targets))
    sends_c, sends_i = [], []
    for k in range(1, n):
        copy = pltpu.make_async_remote_copy(
            cot_v, cot_g.at[me], cs.at[k], cr.at[k], device_id={"fs": fs_peer[k]}
        )
        copy.start()
        sends_c.append(copy)
    for k in range(1, n):
        copy = pltpu.make_async_remote_copy(
            in_v, in_g.at[me], is_.at[k], ir.at[k], device_id={"fs": fs_peer[k]}
        )
        copy.start()
        sends_i.append(copy)

    def picker(shape, token_dim):
        t = lax.broadcasted_iota(jnp.int32, shape, token_dim)
        j = lax.broadcasted_iota(jnp.int32, shape, 1 - token_dim)
        q, r = j // SLAB, j % SLAB
        return ((t == q * rows + r) & (r < rows)).astype(F32).astype(BF16)

    pick = picker((tokens, n * SLAB), 0)
    place = picker((n * SLAB, tokens), 1)

    def gathered(ref):
        for s in range(n):
            spread[s * SLAB : s * SLAB + rows, :] = ref[s].astype(F32)
        return dot(pick, spread[...].astype(BF16), NN).astype(BF16)

    own_cot.wait()
    for copy in load_wd:
        copy.wait()
    for copy in sends_c:
        copy.wait_recv()
    cot_out[...] = gathered(cot_g)

    first, other = core * chunks, (1 - core) * chunks
    send1 = []
    for j in range(chunks):
        p1_s[j] = dot(cot_out[...], wd_v[other + j], NT).astype(BF16)
        copy = pltpu.make_async_remote_copy(
            p1_s.at[j], p1_r.at[j], s1.at[j], r1.at[j], device_id={"tp": partner}
        )
        copy.start()
        send1.append(copy)
    for j in range(chunks):
        own[j] = dot(cot_out[...], wd_v[first + j], NT)
    send2 = []
    for j in range(chunks):
        send1[j].wait_recv()
        total = own[j] + p1_r[j].astype(F32)
        own[j] = total
        p2_s[j] = total.astype(BF16)
        for k in range(1, chips):
            copy = pltpu.make_async_remote_copy(
                p2_s.at[j],
                p2_r.at[k - 1, j],
                s2.at[k - 1, j],
                r2.at[k - 1, j],
                device_id={"tp": x_peer[k]},
            )
            copy.start()
            send2.append(copy)

    own_in.wait()
    for copy in sends_i:
        copy.wait_recv()
    in_out[...] = gathered(in_g)
    for copy in load_pre:
        copy.wait()
    for copy in load_wu:
        copy.wait()

    send3 = []
    for j in range(chunks):
        hidden = own[j]
        for k in range(1, chips):
            send2[j * (chips - 1) + k - 1].wait_recv()
            hidden = hidden + p2_r[k - 1, j].astype(F32)
        active = jnp.maximum(pre_v[first + j].astype(F32), 0.0)
        gp_out[first + j] = (2.0 * active * hidden).astype(BF16)
        copy = pltpu.make_async_remote_copy(
            gp_out.at[first + j],
            gp_out.at[first + j],
            s3.at[j],
            r3.at[j],
            device_id={"tp": partner},
        )
        copy.start()
        send3.append(copy)
    acc = None
    for j in range(chunks):
        term = dot(gp_out[first + j], wu_v[first + j], NT)
        acc = term if acc is None else acc + term
    for j in range(chunks):
        pltpu.make_async_remote_copy(
            gp_out.at[other + j],
            gp_out.at[other + j],
            s3.at[j],
            r3.at[j],
            device_id={"tp": partner},
        ).wait_recv()
        acc = acc + dot(gp_out[other + j], wu_v[other + j], NT)
    slabs = dot(place, acc.astype(BF16), NN)
    for s in range(n):
        rs_s[s] = slabs[s * SLAB : s * SLAB + rows, :].astype(BF16)
    send4 = []
    for k in range(1, n):
        copy = pltpu.make_async_remote_copy(
            rs_s.at[fs_peer[k]],
            rs_r.at[k - 1],
            s4.at[k],
            r4.at[k],
            device_id={"fs": fs_peer[k]},
        )
        copy.start()
        send4.append(copy)
    for copy in sends_c + sends_i + send1 + send2 + send3:
        copy.wait_send()
    total = rs_s[me].astype(F32)
    for k in range(1, n):
        send4[k - 1].wait_recv()
        total = total + rs_r[k - 1].astype(F32)
    gi_out[...] = total.astype(BF16)
    for copy in send4:
        copy.wait_send()


def outer(chunks, cot_ref, in_ref, pre_ref, gp_ref, gi_ref, gi_out, gu_out, gd_out):
    @pl.when(pl.program_id(0) == 0)
    def _():
        gi_out[...] = gi_ref[...]

    active = jnp.maximum(pre_ref[...].astype(F32), 0.0)
    act = (active * active).astype(BF16)
    gd_out[...] = dot(act, cot_ref[...], TN)
    width = gp_ref.shape[2]
    for j in range(2 * chunks):
        gu_out[:, j * width : (j + 1) * width] = dot(in_ref[...], gp_ref[j], TN)


def fused(n, ntp, inputs, cotangent, pre_act, w_up, w_down):
    rows, d = inputs.shape
    tokens, ff = pre_act.shape
    chips = ntp // 2
    chunks = 2 if (ff // 2) % 256 == 0 else 1
    width = ff // 2 // chunks
    hbm = pl.BlockSpec(memory_space=pl.ANY)
    vmem = pl.BlockSpec(memory_space=pltpu.VMEM)
    dma = pltpu.SemaphoreType.DMA
    cot, full, gp, gi = pl.pallas_call(
        functools.partial(exchange, n, chips, chunks),
        out_shape=(
            jax.ShapeDtypeStruct((tokens, d), BF16),
            jax.ShapeDtypeStruct((tokens, d), BF16),
            jax.ShapeDtypeStruct((2 * chunks, tokens, width), BF16),
            jax.ShapeDtypeStruct((rows, d), BF16),
        ),
        in_specs=[hbm] * 5,
        out_specs=(vmem,) * 4,
        scratch_shapes=[
            pltpu.VMEM((rows, d), BF16),
            pltpu.VMEM((rows, d), BF16),
            pltpu.VMEM((2 * chunks, tokens, width), BF16),
            pltpu.VMEM((2 * chunks, d, width), BF16),
            pltpu.VMEM((2 * chunks, width, d), BF16),
            pltpu.VMEM((n, rows, d), BF16),
            pltpu.VMEM((n, rows, d), BF16),
            pltpu.VMEM((n * SLAB, d), F32),
            pltpu.VMEM((chunks, tokens, width), F32),
            pltpu.VMEM((chunks, tokens, width), BF16),
            pltpu.VMEM((chunks, tokens, width), BF16),
            pltpu.VMEM((chunks, tokens, width), BF16),
            pltpu.VMEM((chips - 1, chunks, tokens, width), BF16),
            pltpu.VMEM((n, rows, d), BF16),
            pltpu.VMEM((n - 1, rows, d), BF16),
            dma((4 + 6 * chunks,)),
            dma((n,)),
            dma((n,)),
            dma((n,)),
            dma((n,)),
            dma((chunks,)),
            dma((chunks,)),
            dma((chips - 1, chunks)),
            dma((chips - 1, chunks)),
            dma((chunks,)),
            dma((chunks,)),
            dma((n,)),
            dma((n,)),
        ],
        compiler_params=pltpu.CompilerParams(collective_id=0, has_side_effects=True),
    )(cotangent, inputs, pre_act, w_up, w_down)
    steps = 8
    fixed = lambda i: (0, 0)
    return pl.pallas_call(
        functools.partial(outer, chunks),
        grid=(steps,),
        out_shape=(
            jax.ShapeDtypeStruct((rows, d), BF16),
            jax.ShapeDtypeStruct((d, ff), F32),
            jax.ShapeDtypeStruct((ff, d), F32),
        ),
        in_specs=[
            pl.BlockSpec((tokens, d), fixed),
            pl.BlockSpec((tokens, d // steps), lambda i: (0, i)),
            pl.BlockSpec((tokens, ff // steps), lambda i: (0, i)),
            pl.BlockSpec((2 * chunks, tokens, width), lambda i: (0, 0, 0)),
            pl.BlockSpec((rows, d), fixed),
        ],
        out_specs=(
            pl.BlockSpec((rows, d), fixed),
            pl.BlockSpec((d // steps, ff), lambda i: (i, 0)),
            pl.BlockSpec((ff // steps, d), lambda i: (i, 0)),
        ),
    )(cot, full, pre_act, gp, gi)


def plain(inputs, cotangent, pre_act, w_up, w_down):
    active = jax.nn.relu(pre_act.astype(F32))
    squared = jnp.square(active).astype(BF16)
    piece = lax.all_gather(cotangent, "fs", axis=0, tiled=True)
    grad_down = dot(squared, piece, TN)
    hidden = lax.psum(dot(piece, w_down, NT).astype(BF16), "tp").astype(F32)
    grad_pre = (2.0 * active * hidden).astype(BF16)
    grad_up = dot(lax.all_gather(inputs, "fs", axis=0, tiled=True), grad_pre, TN)
    grad_input = lax.psum_scatter(
        dot(grad_pre, w_up, NT), "fs", scatter_dimension=0, tiled=True
    ).astype(BF16)
    return (grad_input, grad_up, grad_down)


def solution(mesh):
    n, ntp = mesh.shape["fs"], mesh.shape["tp"]

    def body(inputs, cotangent, pre_act, w_up, w_down):
        rows, d = inputs.shape
        tokens, ff = pre_act.shape
        if (
            1 < n <= 16
            and ntp > 2
            and ntp % 2 == 0
            and rows <= SLAB
            and tokens % 16 == 0
            and d % 1024 == 0
            and ff % 1024 == 0
        ):
            return fused(n, ntp, inputs, cotangent, pre_act, w_up, w_down)
        return plain(inputs, cotangent, pre_act, w_up, w_down)

    return jax.shard_map(
        body,
        mesh=mesh,
        in_specs=(P("fs", "tp"), P("fs", "tp"), P(None, "fs"), P("tp", "fs"), P("fs", "tp")),
        out_specs=(P("fs", "tp"), P("tp", "fs"), P("fs", "tp")),
        check_vma=False,
    )
```

```python
import functools

import jax
import jax.numpy as jnp
from jax import lax
from jax.experimental import pallas as pl
from jax.experimental.pallas import tpu as pltpu
from jax.sharding import PartitionSpec as P

F32, BF16 = jnp.float32, jnp.bfloat16
SLAB = 8
NT = (((1,), (1,)), ((), ()))
TN = (((0,), (0,)), ((), ()))
NN = (((1,), (0,)), ((), ()))


def dot(a, b, dims):
    return lax.dot_general(a, b, dims, preferred_element_type=F32)


def exchange(
    n,
    chips,
    chunks,
    cot_ref,
    in_ref,
    pre_ref,
    wu_ref,
    wd_ref,
    cot_out,
    in_out,
    act_out,
    gp_out,
    gi_out,
    cot_v,
    in_v,
    pre_v,
    wu_v,
    wd_v,
    cot_g,
    in_g,
    spread,
    own,
    p1_s,
    p1_r,
    p2_s,
    p2_r,
    rs_s,
    rs_r,
    local,
    cs,
    cr,
    is_,
    ir,
    s1,
    r1,
    s2,
    r2,
    s3,
    r3,
    s4,
    r4,
):
    me = lax.axis_index("fs")
    tp = lax.axis_index("tp")
    core = lax.rem(tp, 2)
    rows = cot_v.shape[0]
    tokens = n * rows
    width = wd_v.shape[1]
    fs_peer = [None] + [lax.rem(me + k, n) for k in range(1, n)]
    partner = tp + 1 - 2 * core
    x_peer = [None] + [lax.rem(tp + 2 * k, 2 * chips) for k in range(1, chips)]
    targets = (
        [{"fs": p} for p in fs_peer[1:]]
        + [{"tp": partner}]
        + [{"tp": p} for p in x_peer[1:]]
    )

    barrier = pltpu.get_barrier_semaphore()
    for t in targets:
        pl.semaphore_signal(barrier, inc=1, device_id=t)

    load_cot = pltpu.make_async_copy(cot_ref, cot_v, local.at[0])
    load_in = pltpu.make_async_copy(in_ref, in_v, local.at[1])
    load_cot.start()
    load_in.start()
    load_wd, load_pre, load_wu = [], [], []
    for j in range(2 * chunks):
        load_wd.append(
            pltpu.make_async_copy(
                wd_ref.at[pl.ds(j * width, width)], wd_v.at[j], local.at[4 + j]
            )
        )
        load_wd[-1].start()
    for j in range(2 * chunks):
        load_pre.append(
            pltpu.make_async_copy(
                pre_ref.at[:, pl.ds(j * width, width)],
                pre_v.at[j],
                local.at[4 + 2 * chunks + j],
            )
        )
        load_pre[-1].start()
    for j in range(2 * chunks):
        load_wu.append(
            pltpu.make_async_copy(
                wu_ref.at[:, pl.ds(j * width, width)],
                wu_v.at[j],
                local.at[4 + 4 * chunks + j],
            )
        )
        load_wu[-1].start()
    spread[...] = jnp.zeros_like(spread)
    load_cot.wait()
    load_in.wait()
    own_cot = pltpu.make_async_copy(cot_v, cot_g.at[me], local.at[2])
    own_in = pltpu.make_async_copy(in_v, in_g.at[me], local.at[3])
    own_cot.start()
    own_in.start()

    pl.semaphore_wait(barrier, len(targets))
    sends_c, sends_i = [], []
    for k in range(1, n):
        copy = pltpu.make_async_remote_copy(
            cot_v, cot_g.at[me], cs.at[k], cr.at[k], device_id={"fs": fs_peer[k]}
        )
        copy.start()
        sends_c.append(copy)
    for k in range(1, n):
        copy = pltpu.make_async_remote_copy(
            in_v, in_g.at[me], is_.at[k], ir.at[k], device_id={"fs": fs_peer[k]}
        )
        copy.start()
        sends_i.append(copy)

    def picker(shape, token_dim):
        t = lax.broadcasted_iota(jnp.int32, shape, token_dim)
        j = lax.broadcasted_iota(jnp.int32, shape, 1 - token_dim)
        q, r = j // SLAB, j % SLAB
        return ((t == q * rows + r) & (r < rows)).astype(F32).astype(BF16)

    pick = picker((tokens, n * SLAB), 0)
    place = picker((n * SLAB, tokens), 1)

    def gathered(ref):
        for s in range(n):
            spread[s * SLAB : s * SLAB + rows, :] = ref[s].astype(F32)
        return dot(pick, spread[...].astype(BF16), NN).astype(BF16)

    own_cot.wait()
    for copy in load_wd:
        copy.wait()
    for copy in sends_c:
        copy.wait_recv()
    cot_out[...] = gathered(cot_g)

    first, other = core * chunks, (1 - core) * chunks
    send1, send2 = [], []

    def to_partner(j):
        p1_s[j] = dot(cot_out[...], wd_v[other + j], NT).astype(BF16)
        copy = pltpu.make_async_remote_copy(
            p1_s.at[j], p1_r.at[j], s1.at[j], r1.at[j], device_id={"tp": partner}
        )
        copy.start()
        send1.append(copy)

    def to_chips(j):
        send1[j].wait_recv()
        total = own[j] + p1_r[j].astype(F32)
        own[j] = total
        p2_s[j] = total.astype(BF16)
        for k in range(1, chips):
            copy = pltpu.make_async_remote_copy(
                p2_s.at[j],
                p2_r.at[k - 1, j],
                s2.at[k - 1, j],
                r2.at[k - 1, j],
                device_id={"tp": x_peer[k]},
            )
            copy.start()
            send2.append(copy)

    to_partner(0)
    for j in range(chunks):
        own[j] = dot(cot_out[...], wd_v[first + j], NT)
        if j + 1 < chunks:
            to_partner(j + 1)
        to_chips(j)

    own_in.wait()
    for copy in sends_i:
        copy.wait_recv()
    in_out[...] = gathered(in_g)
    for copy in load_pre:
        copy.wait()
    for j in range(2 * chunks):
        active = jnp.maximum(pre_v[j].astype(F32), 0.0)
        act_out[j] = (active * active).astype(BF16)
    for copy in load_wu:
        copy.wait()

    send3 = []
    for j in range(chunks):
        hidden = own[j]
        for k in range(1, chips):
            send2[j * (chips - 1) + k - 1].wait_recv()
            hidden = hidden + p2_r[k - 1, j].astype(F32)
        active = jnp.maximum(pre_v[first + j].astype(F32), 0.0)
        gp_out[first + j] = (2.0 * active * hidden).astype(BF16)
        copy = pltpu.make_async_remote_copy(
            gp_out.at[first + j],
            gp_out.at[first + j],
            s3.at[j],
            r3.at[j],
            device_id={"tp": partner},
        )
        copy.start()
        send3.append(copy)
    acc = None
    for j in range(chunks):
        term = dot(gp_out[first + j], wu_v[first + j], NT)
        acc = term if acc is None else acc + term
    for j in range(chunks):
        pltpu.make_async_remote_copy(
            gp_out.at[other + j],
            gp_out.at[other + j],
            s3.at[j],
            r3.at[j],
            device_id={"tp": partner},
        ).wait_recv()
        acc = acc + dot(gp_out[other + j], wu_v[other + j], NT)
    slabs = dot(place, acc.astype(BF16), NN)
    for s in range(n):
        rs_s[s] = slabs[s * SLAB : s * SLAB + rows, :].astype(BF16)
    send4 = []
    for k in range(1, n):
        copy = pltpu.make_async_remote_copy(
            rs_s.at[fs_peer[k]],
            rs_r.at[k - 1],
            s4.at[k],
            r4.at[k],
            device_id={"fs": fs_peer[k]},
        )
        copy.start()
        send4.append(copy)
    for copy in sends_c + sends_i + send1 + send2 + send3:
        copy.wait_send()
    total = rs_s[me].astype(F32)
    for k in range(1, n):
        send4[k - 1].wait_recv()
        total = total + rs_r[k - 1].astype(F32)
    gi_out[...] = total.astype(BF16)
    for copy in send4:
        copy.wait_send()


def outer(
    chunks, cot_v, in_v, act_v, gp_v, gi_v, gi_out, gu_out, gd_out, gu_v, gd_v, sem
):
    width = gp_v.shape[2]
    pieces = []

    def put(src, dst):
        copy = pltpu.make_async_copy(src, dst, sem.at[len(pieces)])
        copy.start()
        pieces.append(copy)

    half = width // 2
    for j in range(2 * chunks):
        for h in range(2):
            rows = pl.ds(j * width + h * half, half)
            gd_v[rows, :] = dot(act_v[j, :, h * half : (h + 1) * half], cot_v[...], TN)
            put(gd_v.at[rows], gd_out.at[rows])
    put(gi_v, gi_out)
    step = in_v.shape[1] // (4 * chunks)
    for i in range(4 * chunks):
        rows = pl.ds(i * step, step)
        for j in range(2 * chunks):
            gu_v[rows, j * width : (j + 1) * width] = dot(
                in_v[:, i * step : (i + 1) * step], gp_v[j], TN
            )
        put(gu_v.at[rows], gu_out.at[rows])
    for copy in pieces:
        copy.wait()


def fused(n, ntp, inputs, cotangent, pre_act, w_up, w_down):
    rows, d = inputs.shape
    tokens, ff = pre_act.shape
    chips = ntp // 2
    chunks = 2 if (ff // 2) % 256 == 0 else 1
    width = ff // 2 // chunks
    hbm = pl.BlockSpec(memory_space=pl.ANY)
    vmem = pl.BlockSpec(memory_space=pltpu.VMEM)
    dma = pltpu.SemaphoreType.DMA
    cot, full, act, gp, gi = pl.pallas_call(
        functools.partial(exchange, n, chips, chunks),
        out_shape=(
            pltpu.VMEM((tokens, d), BF16),
            pltpu.VMEM((tokens, d), BF16),
            pltpu.VMEM((2 * chunks, tokens, width), BF16),
            pltpu.VMEM((2 * chunks, tokens, width), BF16),
            pltpu.VMEM((rows, d), BF16),
        ),
        in_specs=[hbm] * 5,
        out_specs=(vmem,) * 5,
        scratch_shapes=[
            pltpu.VMEM((rows, d), BF16),
            pltpu.VMEM((rows, d), BF16),
            pltpu.VMEM((2 * chunks, tokens, width), BF16),
            pltpu.VMEM((2 * chunks, d, width), BF16),
            pltpu.VMEM((2 * chunks, width, d), BF16),
            pltpu.VMEM((n, rows, d), BF16),
            pltpu.VMEM((n, rows, d), BF16),
            pltpu.VMEM((n * SLAB, d), F32),
            pltpu.VMEM((chunks, tokens, width), F32),
            pltpu.VMEM((chunks, tokens, width), BF16),
            pltpu.VMEM((chunks, tokens, width), BF16),
            pltpu.VMEM((chunks, tokens, width), BF16),
            pltpu.VMEM((chips - 1, chunks, tokens, width), BF16),
            pltpu.VMEM((n, rows, d), BF16),
            pltpu.VMEM((n - 1, rows, d), BF16),
            dma((4 + 6 * chunks,)),
            dma((n,)),
            dma((n,)),
            dma((n,)),
            dma((n,)),
            dma((chunks,)),
            dma((chunks,)),
            dma((chips - 1, chunks)),
            dma((chips - 1, chunks)),
            dma((chunks,)),
            dma((chunks,)),
            dma((n,)),
            dma((n,)),
        ],
        compiler_params=pltpu.CompilerParams(collective_id=0, has_side_effects=True),
    )(cotangent, inputs, pre_act, w_up, w_down)
    return pl.pallas_call(
        functools.partial(outer, chunks),
        out_shape=(
            jax.ShapeDtypeStruct((rows, d), BF16),
            jax.ShapeDtypeStruct((d, ff), F32),
            jax.ShapeDtypeStruct((ff, d), F32),
        ),
        in_specs=[vmem] * 5,
        out_specs=(hbm,) * 3,
        scratch_shapes=[
            pltpu.VMEM((d, ff), F32),
            pltpu.VMEM((ff, d), F32),
            dma((8 * chunks + 1,)),
        ],
    )(*(pltpu.with_memory_space_constraint(x, pltpu.VMEM) for x in (cot, full, act, gp, gi)))


def plain(inputs, cotangent, pre_act, w_up, w_down):
    active = jax.nn.relu(pre_act.astype(F32))
    squared = jnp.square(active).astype(BF16)
    piece = lax.all_gather(cotangent, "fs", axis=0, tiled=True)
    grad_down = dot(squared, piece, TN)
    hidden = lax.psum(dot(piece, w_down, NT).astype(BF16), "tp").astype(F32)
    grad_pre = (2.0 * active * hidden).astype(BF16)
    grad_up = dot(lax.all_gather(inputs, "fs", axis=0, tiled=True), grad_pre, TN)
    grad_input = lax.psum_scatter(
        dot(grad_pre, w_up, NT), "fs", scatter_dimension=0, tiled=True
    ).astype(BF16)
    return (grad_input, grad_up, grad_down)


def solution(mesh):
    n, ntp = mesh.shape["fs"], mesh.shape["tp"]

    def body(inputs, cotangent, pre_act, w_up, w_down):
        rows, d = inputs.shape
        tokens, ff = pre_act.shape
        if (
            1 < n <= 16
            and ntp > 2
            and ntp % 2 == 0
            and rows <= SLAB
            and tokens % 16 == 0
            and d % 1024 == 0
            and ff % 1024 == 0
        ):
            return fused(n, ntp, inputs, cotangent, pre_act, w_up, w_down)
        return plain(inputs, cotangent, pre_act, w_up, w_down)

    return jax.shard_map(
        body,
        mesh=mesh,
        in_specs=(P("fs", "tp"), P("fs", "tp"), P(None, "fs"), P("tp", "fs"), P("fs", "tp")),
        out_specs=(P("fs", "tp"), P("tp", "fs"), P("fs", "tp")),
        check_vma=False,
    )
```

```python
import functools

import jax
import jax.numpy as jnp
from jax import lax
from jax.experimental import pallas as pl
from jax.experimental.pallas import tpu as pltpu
from jax.sharding import PartitionSpec as P

F32, BF16 = jnp.float32, jnp.bfloat16
SLAB = 8
NT = (((1,), (1,)), ((), ()))
TN = (((0,), (0,)), ((), ()))
NN = (((1,), (0,)), ((), ()))


def dot(a, b, dims):
    return lax.dot_general(a, b, dims, preferred_element_type=F32)


def exchange(
    n,
    chips,
    chunks,
    cot_ref,
    in_ref,
    pre_ref,
    wu_ref,
    wd_ref,
    cot_out,
    in_out,
    act_out,
    gp_out,
    gi_out,
    cot_v,
    in_v,
    pre_v,
    wu_v,
    wd_v,
    cot_g,
    in_g,
    spread,
    own,
    p1_s,
    p1_r,
    p2_s,
    p2_r,
    rs_s,
    rs_r,
    local,
    cs,
    cr,
    is_,
    ir,
    s1,
    r1,
    s2,
    r2,
    s3,
    r3,
    s4,
    r4,
):
    me = lax.axis_index("fs")
    tp = lax.axis_index("tp")
    core = lax.rem(tp, 2)
    rows = cot_v.shape[0]
    tokens = n * rows
    width = wd_v.shape[1]
    fs_peer = [None] + [lax.rem(me + k, n) for k in range(1, n)]
    partner = tp + 1 - 2 * core
    x_peer = [None] + [lax.rem(tp + 2 * k, 2 * chips) for k in range(1, chips)]
    targets = (
        [{"fs": p} for p in fs_peer[1:]]
        + [{"tp": partner}]
        + [{"tp": p} for p in x_peer[1:]]
    )

    barrier = pltpu.get_barrier_semaphore()
    for t in targets:
        pl.semaphore_signal(barrier, inc=1, device_id=t)

    load_cot = pltpu.make_async_copy(cot_ref, cot_v, local.at[0])
    load_in = pltpu.make_async_copy(in_ref, in_v, local.at[1])
    load_cot.start()
    load_in.start()
    load_wd, load_pre, load_wu = [], [], []
    for j in range(2 * chunks):
        load_wd.append(
            pltpu.make_async_copy(
                wd_ref.at[pl.ds(j * width, width)], wd_v.at[j], local.at[4 + j]
            )
        )
        load_wd[-1].start()
    for j in range(2 * chunks):
        load_pre.append(
            pltpu.make_async_copy(
                pre_ref.at[:, pl.ds(j * width, width)],
                pre_v.at[j],
                local.at[4 + 2 * chunks + j],
            )
        )
        load_pre[-1].start()
    for j in range(2 * chunks):
        load_wu.append(
            pltpu.make_async_copy(
                wu_ref.at[:, pl.ds(j * width, width)],
                wu_v.at[j],
                local.at[4 + 4 * chunks + j],
            )
        )
        load_wu[-1].start()
    spread[...] = jnp.zeros_like(spread)
    load_cot.wait()
    load_in.wait()
    own_cot = pltpu.make_async_copy(cot_v, cot_g.at[me], local.at[2])
    own_in = pltpu.make_async_copy(in_v, in_g.at[me], local.at[3])
    own_cot.start()
    own_in.start()

    pl.semaphore_wait(barrier, len(targets))
    sends_c, sends_i = [], []
    for k in range(1, n):
        copy = pltpu.make_async_remote_copy(
            cot_v, cot_g.at[me], cs.at[k], cr.at[k], device_id={"fs": fs_peer[k]}
        )
        copy.start()
        sends_c.append(copy)
    def picker(shape, token_dim):
        t = lax.broadcasted_iota(jnp.int32, shape, token_dim)
        j = lax.broadcasted_iota(jnp.int32, shape, 1 - token_dim)
        q, r = j // SLAB, j % SLAB
        return ((t == q * rows + r) & (r < rows)).astype(F32).astype(BF16)

    pick = picker((tokens, n * SLAB), 0)
    place = picker((n * SLAB, tokens), 1)

    def gathered(ref):
        for s in range(n):
            spread[s * SLAB : s * SLAB + rows, :] = ref[s].astype(F32)
        return dot(pick, spread[...].astype(BF16), NN).astype(BF16)

    own_cot.wait()
    for copy in load_wd:
        copy.wait()
    for copy in sends_c:
        copy.wait_recv()
    cot_out[...] = gathered(cot_g)

    first, other = core * chunks, (1 - core) * chunks
    send1, send2 = [], []

    def to_partner(j):
        p1_s[j] = dot(cot_out[...], wd_v[other + j], NT).astype(BF16)
        copy = pltpu.make_async_remote_copy(
            p1_s.at[j], p1_r.at[j], s1.at[j], r1.at[j], device_id={"tp": partner}
        )
        copy.start()
        send1.append(copy)

    def to_chips(j):
        send1[j].wait_recv()
        total = own[j] + p1_r[j].astype(F32)
        own[j] = total
        p2_s[j] = total.astype(BF16)
        for k in range(1, chips):
            copy = pltpu.make_async_remote_copy(
                p2_s.at[j],
                p2_r.at[k - 1, j],
                s2.at[k - 1, j],
                r2.at[k - 1, j],
                device_id={"tp": x_peer[k]},
            )
            copy.start()
            send2.append(copy)

    to_partner(0)
    for k in range(1, n):
        copy = pltpu.make_async_remote_copy(
            in_v, in_g.at[me], is_.at[k], ir.at[k], device_id={"fs": fs_peer[k]}
        )
        copy.start()
        sends_i.append(copy)
    for j in range(chunks):
        own[j] = dot(cot_out[...], wd_v[first + j], NT)
        if j + 1 < chunks:
            to_partner(j + 1)
        to_chips(j)

    own_in.wait()
    for copy in sends_i:
        copy.wait_recv()
    in_out[...] = gathered(in_g)
    for copy in load_pre:
        copy.wait()
    for j in range(2 * chunks):
        active = jnp.maximum(pre_v[j].astype(F32), 0.0)
        act_out[j] = (active * active).astype(BF16)
    for copy in load_wu:
        copy.wait()

    send3 = []
    for j in range(chunks):
        hidden = own[j]
        for k in range(1, chips):
            send2[j * (chips - 1) + k - 1].wait_recv()
            hidden = hidden + p2_r[k - 1, j].astype(F32)
        active = jnp.maximum(pre_v[first + j].astype(F32), 0.0)
        gp_out[first + j] = (2.0 * active * hidden).astype(BF16)
        copy = pltpu.make_async_remote_copy(
            gp_out.at[first + j],
            gp_out.at[first + j],
            s3.at[j],
            r3.at[j],
            device_id={"tp": partner},
        )
        copy.start()
        send3.append(copy)
    acc = None
    for j in range(chunks):
        term = dot(gp_out[first + j], wu_v[first + j], NT)
        acc = term if acc is None else acc + term
    for j in range(chunks):
        pltpu.make_async_remote_copy(
            gp_out.at[other + j],
            gp_out.at[other + j],
            s3.at[j],
            r3.at[j],
            device_id={"tp": partner},
        ).wait_recv()
        acc = acc + dot(gp_out[other + j], wu_v[other + j], NT)
    slabs = dot(place, acc.astype(BF16), NN)
    for s in range(n):
        rs_s[s] = slabs[s * SLAB : s * SLAB + rows, :].astype(BF16)
    send4 = []
    for k in range(1, n):
        copy = pltpu.make_async_remote_copy(
            rs_s.at[fs_peer[k]],
            rs_r.at[k - 1],
            s4.at[k],
            r4.at[k],
            device_id={"fs": fs_peer[k]},
        )
        copy.start()
        send4.append(copy)
    for copy in sends_c + sends_i + send1 + send2 + send3:
        copy.wait_send()
    total = rs_s[me].astype(F32)
    for k in range(1, n):
        send4[k - 1].wait_recv()
        total = total + rs_r[k - 1].astype(F32)
    gi_out[...] = total.astype(BF16)
    for copy in send4:
        copy.wait_send()


def outer(
    chunks, cot_v, in_v, act_v, gp_v, gi_v, gi_out, gu_out, gd_out, gu_v, gd_v, sem
):
    width = gp_v.shape[2]
    pieces = []

    def put(src, dst):
        copy = pltpu.make_async_copy(src, dst, sem.at[len(pieces)])
        copy.start()
        pieces.append(copy)

    half = width // 2
    for j in range(2 * chunks):
        for h in range(2):
            rows = pl.ds(j * width + h * half, half)
            gd_v[rows, :] = dot(act_v[j, :, h * half : (h + 1) * half], cot_v[...], TN)
            put(gd_v.at[rows], gd_out.at[rows])
    put(gi_v, gi_out)
    step = in_v.shape[1] // (4 * chunks)
    for i in range(4 * chunks):
        rows = pl.ds(i * step, step)
        for j in range(2 * chunks):
            gu_v[rows, j * width : (j + 1) * width] = dot(
                in_v[:, i * step : (i + 1) * step], gp_v[j], TN
            )
        put(gu_v.at[rows], gu_out.at[rows])
    for copy in pieces:
        copy.wait()


def fused(n, ntp, inputs, cotangent, pre_act, w_up, w_down):
    rows, d = inputs.shape
    tokens, ff = pre_act.shape
    chips = ntp // 2
    chunks = 2 if (ff // 2) % 256 == 0 else 1
    width = ff // 2 // chunks
    hbm = pl.BlockSpec(memory_space=pl.ANY)
    vmem = pl.BlockSpec(memory_space=pltpu.VMEM)
    dma = pltpu.SemaphoreType.DMA
    cot, full, act, gp, gi = pl.pallas_call(
        functools.partial(exchange, n, chips, chunks),
        out_shape=(
            pltpu.VMEM((tokens, d), BF16),
            pltpu.VMEM((tokens, d), BF16),
            pltpu.VMEM((2 * chunks, tokens, width), BF16),
            pltpu.VMEM((2 * chunks, tokens, width), BF16),
            pltpu.VMEM((rows, d), BF16),
        ),
        in_specs=[hbm] * 5,
        out_specs=(vmem,) * 5,
        scratch_shapes=[
            pltpu.VMEM((rows, d), BF16),
            pltpu.VMEM((rows, d), BF16),
            pltpu.VMEM((2 * chunks, tokens, width), BF16),
            pltpu.VMEM((2 * chunks, d, width), BF16),
            pltpu.VMEM((2 * chunks, width, d), BF16),
            pltpu.VMEM((n, rows, d), BF16),
            pltpu.VMEM((n, rows, d), BF16),
            pltpu.VMEM((n * SLAB, d), F32),
            pltpu.VMEM((chunks, tokens, width), F32),
            pltpu.VMEM((chunks, tokens, width), BF16),
            pltpu.VMEM((chunks, tokens, width), BF16),
            pltpu.VMEM((chunks, tokens, width), BF16),
            pltpu.VMEM((chips - 1, chunks, tokens, width), BF16),
            pltpu.VMEM((n, rows, d), BF16),
            pltpu.VMEM((n - 1, rows, d), BF16),
            dma((4 + 6 * chunks,)),
            dma((n,)),
            dma((n,)),
            dma((n,)),
            dma((n,)),
            dma((chunks,)),
            dma((chunks,)),
            dma((chips - 1, chunks)),
            dma((chips - 1, chunks)),
            dma((chunks,)),
            dma((chunks,)),
            dma((n,)),
            dma((n,)),
        ],
        compiler_params=pltpu.CompilerParams(collective_id=0, has_side_effects=True),
    )(cotangent, inputs, pre_act, w_up, w_down)
    return pl.pallas_call(
        functools.partial(outer, chunks),
        out_shape=(
            jax.ShapeDtypeStruct((rows, d), BF16),
            jax.ShapeDtypeStruct((d, ff), F32),
            jax.ShapeDtypeStruct((ff, d), F32),
        ),
        in_specs=[vmem] * 5,
        out_specs=(hbm,) * 3,
        scratch_shapes=[
            pltpu.VMEM((d, ff), F32),
            pltpu.VMEM((ff, d), F32),
            dma((8 * chunks + 1,)),
        ],
    )(*(pltpu.with_memory_space_constraint(x, pltpu.VMEM) for x in (cot, full, act, gp, gi)))


def plain(inputs, cotangent, pre_act, w_up, w_down):
    active = jax.nn.relu(pre_act.astype(F32))
    squared = jnp.square(active).astype(BF16)
    piece = lax.all_gather(cotangent, "fs", axis=0, tiled=True)
    grad_down = dot(squared, piece, TN)
    hidden = lax.psum(dot(piece, w_down, NT).astype(BF16), "tp").astype(F32)
    grad_pre = (2.0 * active * hidden).astype(BF16)
    grad_up = dot(lax.all_gather(inputs, "fs", axis=0, tiled=True), grad_pre, TN)
    grad_input = lax.psum_scatter(
        dot(grad_pre, w_up, NT), "fs", scatter_dimension=0, tiled=True
    ).astype(BF16)
    return (grad_input, grad_up, grad_down)


def solution(mesh):
    n, ntp = mesh.shape["fs"], mesh.shape["tp"]

    def body(inputs, cotangent, pre_act, w_up, w_down):
        rows, d = inputs.shape
        tokens, ff = pre_act.shape
        if (
            1 < n <= 16
            and ntp > 2
            and ntp % 2 == 0
            and rows <= SLAB
            and tokens % 16 == 0
            and d % 1024 == 0
            and ff % 1024 == 0
        ):
            return fused(n, ntp, inputs, cotangent, pre_act, w_up, w_down)
        return plain(inputs, cotangent, pre_act, w_up, w_down)

    return jax.shard_map(
        body,
        mesh=mesh,
        in_specs=(P("fs", "tp"), P("fs", "tp"), P(None, "fs"), P("tp", "fs"), P("fs", "tp")),
        out_specs=(P("fs", "tp"), P("tp", "fs"), P("fs", "tp")),
        check_vma=False,
    )
```
